32 devices in a mesh: sp: 8 (over z, x), tp: 4 (over y, core).
Axes of the slice: x: 2, y: 2, z: 4, core: 2. Of those that a mesh axis runs over, the one named last changes fastest.
Arguments:
- conv_in: bfloat16 [6144, 1024], P('sp', 'tp'), may hold values from -6 to 6
- conv_pre: bfloat16 [6144, 1024], P('sp', 'tp'), may hold values from -6 to 6
- conv_post: bfloat16 [6144, 1024], P('sp', 'tp'), may hold values from -6 to 6
- taps: float32 [3, 1024], P(None, 'tp'), may hold values from -3 to 3
- out_proj: bfloat16 [1024, 2048], P('tp'), may hold values from -0.1875 to 0.1875
- stream: bfloat16 [6144, 2048], P(('sp', 'tp')), may hold values from -6 to 6
- norm_gain: float32 [2048], replicated, may hold values from 0.1 to 1.9
- routes: int32 [6144, 2], P(('sp', 'tp')), may hold values from 0 to 7, all different within a row; in each aligned block of 192 rows (0 to 191, 192 to 383, ...) at most 64 rows name the same one
- route_weight: float32 [6144, 2], P(('sp', 'tp')), may hold values from 0.1 to 1
- gate_w: bfloat16 [8, 2048, 2048], P('sp', None, 'tp'), may hold values from -0.52734375 to 0.52734375
- up_w: bfloat16 [8, 2048, 2048], P('sp', None, 'tp'), may hold values from -0.52734375 to 0.52734375
- down_w: bfloat16 [8, 2048, 2048], P('sp', 'tp'), may hold values from -0.013244629 to 0.013244629
Outputs:
- output: bfloat16 [6144, 2048], P(('sp', 'tp'))
The draws below stay inside these ranges and needn't reach their ends.
Inputs may be any that keep to these rules, and one draw needn't show every extreme that they name: `routes`: each row names 2 different experts. In each aligned block of 192 rows no expert is named more than 64 times, a bound that some block reaches.
All inputs are finite; a program needn't handle non-finite values.
Results may differ from the reference program's by a relative error of at most 0.015.
Values may be sent and summed in bfloat16 or wider, within the bound.
A program may use at most 128 MiB of HBM per device.

```python
import math
import jax
import jax.numpy as jnp
import numpy as np
from jax import lax

D = 2048
CONV = 1024
FF = 2048
TOP = 2
EXPERTS = 8
TOK_DEV = 192
CAP = 64
TOKENS = 6144
N_TP = 4


def block_levels(rng, shape, pieces, low, top_value):
    level = 1.0
    for axis_at, parts in pieces:
        draws = jax.random.uniform(jax.random.fold_in(jax.random.fold_in(rng, 6), axis_at), (parts,), jnp.float32, low / len(pieces), top_value / len(pieces))
        level = level * jnp.repeat(jnp.exp(draws), shape[axis_at] // parts).reshape((-1,) + (1,) * (len(shape) - 1 - axis_at))
    return level


def deal_out(stream_key, own, number, rows, number_of, top, limit, lean):
    sequence = jax.random.permutation(stream_key, number_of)
    crowded, ordinary = load_shares(number_of, rows * top, limit, lean, True), load_shares(number_of, rows * top, limit, lean, False)
    places = jnp.arange(number_of)

    def named(tallies, offset_by):
        used = int((tallies > 0).sum())
        fixed = max(1, used // 4)
        moved = fixed + (places - fixed + offset_by * (used - fixed)) % max(1, number_of - fixed)
        return jnp.zeros((number_of,), jnp.int32).at[sequence[jnp.where(places < fixed, places, moved)]].set(jnp.asarray(tallies, jnp.int32))

    tallies = jnp.where(number % 4 == 0, named(crowded, number // 4), named(ordinary, number - number // 4 - 1))
    mixed = jax.random.permutation(jax.random.fold_in(own, 3), number_of)
    donor, sink = mixed[0:number_of // 2 * 2:2], mixed[1:number_of // 2 * 2:2]
    room = jnp.minimum(tallies[donor] - 1, limit - tallies[sink]) // 2
    room = jnp.where((donor == sequence[0]) | (sink == sequence[0]) | (tallies[sink] == 0), 0, jnp.maximum(room, 0))
    moved = jax.random.randint(jax.random.fold_in(own, 4), (number_of // 2,), 0, 1 << 20) % (room + 1)
    tallies = tallies.at[donor].add(-moved).at[sink].add(moved)
    items = jnp.searchsorted(jnp.cumsum(tallies), jnp.arange(rows * top), side="right").astype(jnp.int32)
    grid = items.reshape(top, rows).T
    grid = grid[jax.random.permutation(jax.random.fold_in(own, 1), rows)]
    offset_by = jax.random.randint(jax.random.fold_in(own, 2), (rows, 1), 0, top)
    return jnp.take_along_axis(grid, (jnp.arange(top)[None, :] + offset_by) % top, axis=1)


def load_shares(amount, total, most, lean, full):
    portions = [(1 << 20) // math.isqrt(standing ** lean) + 1 for standing in range(1, amount + 1)]
    largest = most if full else min(most, max(-(-total // amount), total * portions[0] // sum(portions)))
    least = 1 if total - largest >= amount - 1 else 0
    holding, rest = [largest] + [least] * (amount - 1), total - largest - least * (amount - 1)
    while rest > 0:
        candidates = [i for i in range(1, amount) if holding[i] < largest] or [i for i in range(1, amount) if holding[i] < most]
        pool, budget = sum([portions[i] for i in candidates]), rest
        for i in candidates:
            more = min(most - holding[i], max(1, budget * portions[i] // pool), rest)
            holding[i] = holding[i] + more
            rest = rest - more
    return np.array(holding)


def centred(key, extent, width, bound, pieces=(), kind=jnp.bfloat16):
    level = block_levels(key, extent, pieces, -0.22, 0.18) if pieces else 1.0
    array = jax.random.normal(key, extent, jnp.float32) * width * level
    return jnp.minimum(jnp.maximum(array, -bound), bound).astype(kind)


def setup_inputs(seed: int = 0) -> dict:
    key_of = jax.random.split(jax.random.key(seed), 13)
    conv_in = centred(key_of[0], (TOKENS, CONV), 1.0, 6.0, ((0, 8), (1, 4)))
    conv_pre = centred(key_of[1], (TOKENS, CONV), 1.0, 6.0, ((0, 8), (1, 4)))
    conv_post = centred(key_of[2], (TOKENS, CONV), 1.0, 6.0, ((0, 8), (1, 4)))
    taps = centred(key_of[3], (3, CONV), 0.58, 3.0, ((1, 4),), jnp.float32)
    out_proj = centred(key_of[4], (CONV, D), CONV ** -0.5, 0.1875, ((0, 4),))
    stream = centred(key_of[5], (TOKENS, D), 1.0, 6.0, ((0, 32),))
    norm_gain = jnp.clip(1.0 + 0.18 * jax.random.normal(key_of[6], (D,), jnp.float32), 0.1, 1.9)
    routes_keys = jax.random.split(jax.random.fold_in(key_of[7], 1), TOKENS // TOK_DEV)
    routes_turns = jax.random.permutation(jax.random.fold_in(key_of[7], 3), TOKENS // TOK_DEV)
    routes = jax.vmap(lambda own, number: deal_out(jax.random.fold_in(key_of[7], 2), own, number, TOK_DEV, EXPERTS, TOP, CAP, 1))(routes_keys, routes_turns).reshape((TOKENS, TOP))
    route_weight = jnp.clip(jnp.exp(math.log(1.0) - 2.3025851 * jax.random.uniform(key_of[8], (TOKENS, TOP), jnp.float32) ** block_levels(key_of[8], (TOKENS, TOP), ((0, 32),), -0.2, 0.2)), 0.1, 1.0)
    gate_w = centred(key_of[9], (EXPERTS, D, FF), (4 * D ** -0.5), 0.52734375, ((0, 8), (2, 4)))
    up_w = centred(key_of[10], (EXPERTS, D, FF), (4 * D ** -0.5), 0.52734375, ((0, 8), (2, 4)))
    down_w = centred(key_of[11], (EXPERTS, FF, D), (0.1 * FF ** -0.5), 0.013244629, ((0, 8), (1, 4)))
    return {"conv_in": conv_in, "conv_pre": conv_pre, "conv_post": conv_post, "taps": taps, "out_proj": out_proj, "stream": stream, "norm_gain": norm_gain, "routes": routes, "route_weight": route_weight, "gate_w": gate_w, "up_w": up_w, "down_w": down_w}


EPSILON = 1e-05
LIMIT = 7.0
ALPHA = 1.702

def clamped_unit(gate_pre, up_pre):
    gated = jnp.minimum(gate_pre, LIMIT)
    upward = jnp.clip(up_pre, -LIMIT, LIMIT)
    return (upward + 1.0) * gated * jax.nn.sigmoid(ALPHA * gated)

def block_ranks(chosen, block_rows, count):
    shaped = chosen.reshape(-1, block_rows)
    onehot = (shaped[:, :, None] == jnp.arange(count, dtype=jnp.int32)[None, None, :]).astype(jnp.int32)
    running = jnp.cumsum(onehot, axis=1) - 1
    return lax.optimization_barrier(jnp.sum(running * onehot, axis=2)).reshape(-1).astype(jnp.int32)

def reference(conv_in, conv_pre, conv_post, taps, out_proj, stream, norm_gain, routes, route_weight, gate_w, up_w, down_w):
    product = conv_pre.astype(jnp.float32) * conv_in.astype(jnp.float32)
    padded = jnp.pad(product, ((1, 1), (0, 0)))
    convolved = taps[0] * padded[:-2] + taps[1] * padded[1:-1] + taps[2] * padded[2:]
    mixed = (conv_post.astype(jnp.float32) * convolved).astype(jnp.bfloat16)
    branch = jnp.dot(mixed, out_proj, preferred_element_type=jnp.float32)
    resid = (stream.astype(jnp.float32) + branch).astype(jnp.bfloat16)
    resid_f = resid.astype(jnp.float32)
    scale = lax.rsqrt(lax.optimization_barrier(jnp.mean(resid_f * resid_f, axis=-1, keepdims=True)) + EPSILON)
    normed = (resid_f * scale * norm_gain).astype(jnp.bfloat16)
    chosen = routes.reshape(-1)
    ranks = block_ranks(chosen, TOK_DEV * TOP, EXPERTS)
    entry_ids = jnp.arange(chosen.shape[0], dtype=jnp.int32)
    slot_ids = entry_ids // (TOK_DEV * TOP) * CAP + ranks
    token_ids = entry_ids // TOP
    slots_all = TOKENS // TOK_DEV * CAP
    buffer = jnp.zeros((EXPERTS, slots_all, D), jnp.bfloat16).at[chosen, slot_ids].set(normed[token_ids])
    part_width = FF // N_TP

    def expert_pass(operands):
        rows_in, gate_one, up_one, down_one = operands
        gate_pre = jnp.dot(rows_in, gate_one, preferred_element_type=jnp.float32)
        up_pre = jnp.dot(rows_in, up_one, preferred_element_type=jnp.float32)
        active = clamped_unit(gate_pre, up_pre).astype(jnp.bfloat16)
        summed = jnp.zeros((rows_in.shape[0], D), jnp.float32)
        for portion in range(N_TP):
            lower = portion * part_width
            piece = jnp.dot(active[:, lower:lower + part_width], down_one[lower:lower + part_width], preferred_element_type=jnp.float32).astype(jnp.bfloat16)
            summed = summed + piece.astype(jnp.float32)
        return summed.astype(jnp.bfloat16)
    results = lax.map(expert_pass, (buffer, gate_w, up_w, down_w))
    picked = results[chosen, slot_ids].reshape(TOKENS, TOP, D)
    total = resid.astype(jnp.float32)
    for column in range(TOP):
        total = total + route_weight[:, column:column + 1] * picked[:, column].astype(jnp.float32)
    return total.astype(jnp.bfloat16)
```

```python
import functools

import jax
import jax.numpy as jnp
from jax import lax
from jax.experimental import pallas as pl
from jax.experimental.pallas import tpu as pltpu
from jax.sharding import PartitionSpec as P

EPSILON = 1e-05
LIMIT = 7.0
ALPHA = 1.702


def with_halo(x, sides, width):
    for axis, dim in sides:
        count, length = (lax.axis_size(axis), x.shape[dim])
        up = [(i, (i + 1) % count) for i in range(count - 1)]
        down = [(j, i) for i, j in up]
        last = lax.slice_in_dim(x, length - width, length, axis=dim)
        first = lax.slice_in_dim(x, 0, width, axis=dim)
        before = lax.ppermute(last, axis, up)
        after = lax.ppermute(first, axis, down)
        x = jnp.concatenate([before, x, after], axis=dim)
    return x

MESH = pl.DeviceIdType.MESH


def clamped_unit(gate_pre, up_pre):
    gated = jnp.minimum(gate_pre, LIMIT)
    upward = jnp.clip(up_pre, -LIMIT, LIMIT)
    return (upward + 1.0) * gated * jax.nn.sigmoid(ALPHA * gated)


def experts_kernel(
    n,
    group,
    disp,
    gate_w,
    up_w,
    down_w,
    out,
    rows,
    parts,
    partner_parts,
    chip_sum,
    peer_sum,
    final,
    gate_v,
    up_v,
    down_v,
    w_sem,
    own_sem,
    sp_send,
    sp_recv,
    pair_send,
    pair_recv,
    peer_send,
    peer_recv,
    fwd_send,
    fwd_recv,
    part_send,
    part_recv,
    sum_send,
    sum_recv,
    ret_send,
    ret_recv,
):
    steps = n // group
    me = lax.axis_index("sp")
    quarter = lax.axis_index("tp")
    y, c = quarter // 2, quarter % 2
    partner = {"tp": y * 2 + 1 - c}
    peer = {"tp": (1 - y) * 2 + c}

    def remote(source, target, send, recv, device):
        return pltpu.make_async_remote_copy(
            src_ref=source,
            dst_ref=target,
            send_sem=send,
            recv_sem=recv,
            device_id=device,
            device_id_type=MESH,
        )

    loads = [
        pltpu.make_async_copy(gate_w.at[0], gate_v, w_sem.at[0]),
        pltpu.make_async_copy(up_w.at[0], up_v, w_sem.at[1]),
        pltpu.make_async_copy(down_w.at[0], down_v, w_sem.at[2]),
    ]
    own_in = pltpu.make_async_copy(disp.at[me], rows.at[0, c, y, 0], own_sem.at[0])
    own_out = pltpu.make_async_copy(final.at[0, 0], out.at[me], own_sem.at[1])
    own_in.start()
    for load in loads:
        load.start()

    barrier = pltpu.get_barrier_semaphore()

    @pl.loop(1, n)
    def _(j):
        pl.semaphore_signal(barrier, inc=1, device_id={"sp": (me + j) % n}, device_id_type=MESH)

    pl.semaphore_signal(barrier, inc=1, device_id=partner, device_id_type=MESH)
    pl.semaphore_signal(barrier, inc=1, device_id=peer, device_id_type=MESH)
    pl.semaphore_wait(barrier, n + 1)

    def dispatch(j):
        to = (me + n - j) % n
        return remote(
            disp.at[to],
            rows.at[j // group, c, y, j % group],
            sp_send.at[j],
            sp_recv.at[j],
            {"sp": to},
        )

    def pair(t):
        block = rows.at[t, c, y]
        return remote(block, block, pair_send.at[t], pair_recv.at[t], partner)

    def across(t):
        block = rows.at[t, c, y]
        return remote(block, block, peer_send.at[t], peer_recv.at[t], peer)

    def forward(t):
        block = rows.at[t, c, 1 - y]
        return remote(block, block, fwd_send.at[t], fwd_recv.at[t], partner)

    def part(t):
        return remote(
            parts.at[t, 1 - c], partner_parts.at[t], part_send.at[t], part_recv.at[t], partner
        )

    def summed(t):
        return remote(chip_sum.at[t], peer_sum.at[t], sum_send.at[t], sum_recv.at[t], peer)

    def back(j):
        return remote(
            final.at[j // group, j % group],
            out.at[me],
            ret_send.at[j],
            ret_recv.at[j],
            {"sp": (me + j) % n},
        )

    @pl.loop(1, n)
    def _(j):
        dispatch(j).start()

    own_in.wait()
    for load in loads:
        load.wait()
    cap, width = rows.shape[-2:]
    count = 4 * group * cap

    def compute(t):
        x = rows[t].reshape(count, width)
        gate_pre = jnp.dot(x, gate_v[...], preferred_element_type=jnp.float32)
        up_pre = jnp.dot(x, up_v[...], preferred_element_type=jnp.float32)
        active = clamped_unit(gate_pre, up_pre).astype(jnp.bfloat16)
        tile = 512
        for at in range(0, width, tile):
            piece = jnp.dot(active, down_v[:, at : at + tile], preferred_element_type=jnp.float32)
            parts[t, :, :, :, :, at : at + tile] = piece.astype(jnp.bfloat16).reshape(
                2, 2, group, cap, tile
            )

    @pl.loop(0, steps + 4)
    def _(t):
        @pl.when(t < steps)
        def _():
            for g in range(group):
                j = t * group + g

                @pl.when(j > 0)
                def _():
                    dispatch(j).wait_recv()

            across(t).start()
            pair(t).start()

        @pl.when((t >= 1) & (t < steps + 1))
        def _():
            across(t - 1).wait_recv()
            forward(t - 1).start()

        @pl.when((t >= 2) & (t < steps + 2))
        def _():
            pair(t - 2).wait_recv()
            forward(t - 2).wait_recv()
            compute(t - 2)
            part(t - 2).start()

        @pl.when((t >= 3) & (t < steps + 3))
        def _():
            s = t - 3
            part(s).wait_recv()
            chip_sum[s] = (
                parts[s, c, 1 - y].astype(jnp.float32)
                + partner_parts[s, 1 - y].astype(jnp.float32)
            ).astype(jnp.bfloat16)
            summed(s).start()

        @pl.when(t >= 4)
        def _():
            s = t - 4
            summed(s).wait_recv()
            final[s] = (
                parts[s, c, y].astype(jnp.float32)
                + partner_parts[s, y].astype(jnp.float32)
                + peer_sum[s].astype(jnp.float32)
            ).astype(jnp.bfloat16)
            for g in range(group):
                j = s * group + g

                @pl.when(j > 0)
                def _():
                    back(j).start()

                @pl.when(j == 0)
                def _():
                    own_out.start()

    own_out.wait()

    @pl.loop(0, steps)
    def _(t):
        pair(t).wait_send()
        across(t).wait_send()
        forward(t).wait_send()
        part(t).wait_send()
        summed(t).wait_send()

    @pl.loop(1, n)
    def _(j):
        dispatch(j).wait_send()
        back(j).wait()


def run_experts(disp, gate_w, up_w, down_w):
    n, cap, width = disp.shape
    hidden = gate_w.shape[2]
    group = 1
    while n % (2 * group) == 0 and n // group > 8 and 4 * group * cap < 256:
        group *= 2
    steps = n // group
    kind = jnp.bfloat16
    hbm = pl.BlockSpec(memory_space=pltpu.HBM)
    dma = pltpu.SemaphoreType.DMA
    return pl.pallas_call(
        functools.partial(experts_kernel, n, group),
        out_shape=jax.ShapeDtypeStruct((n, cap, width), kind),
        in_specs=[hbm] * 4,
        out_specs=hbm,
        scratch_shapes=[
            pltpu.VMEM((steps, 2, 2, group, cap, width), kind),
            pltpu.VMEM((steps, 2, 2, group, cap, width), kind),
            pltpu.VMEM((steps, 2, group, cap, width), kind),
            pltpu.VMEM((steps, group, cap, width), kind),
            pltpu.VMEM((steps, group, cap, width), kind),
            pltpu.VMEM((steps, group, cap, width), kind),
            pltpu.VMEM((width, hidden), kind),
            pltpu.VMEM((width, hidden), kind),
            pltpu.VMEM((hidden, width), kind),
            dma((3,)),
            dma((2,)),
            dma((n,)),
            dma((n,)),
        ]
        + [dma((steps,))] * 10
        + [dma((n,))] * 2,
        compiler_params=pltpu.CompilerParams(
            collective_id=0, has_side_effects=True, vmem_limit_bytes=60 * 1024 * 1024
        ),
    )(disp, gate_w, up_w, down_w)


def local(
    conv_in,
    conv_pre,
    conv_post,
    taps,
    out_proj,
    stream,
    norm_gain,
    routes,
    route_weight,
    gate_w,
    up_w,
    down_w,
):
    product = conv_pre.astype(jnp.float32) * conv_in.astype(jnp.float32)
    padded = with_halo(product.astype(jnp.bfloat16), (("sp", 0),), 1).astype(product.dtype)
    convolved = taps[0] * padded[:-2] + taps[1] * padded[1:-1] + taps[2] * padded[2:]
    mixed = (conv_post.astype(jnp.float32) * convolved).astype(jnp.bfloat16)
    own_rows = stream.shape[0]
    width = stream.shape[1]
    regrouped = lax.all_to_all(mixed, "tp", split_axis=0, concat_axis=1, tiled=True)
    branch = jnp.dot(
        regrouped,
        lax.all_gather(out_proj, "tp", axis=0, tiled=True),
        preferred_element_type=jnp.float32,
    )
    resid = (stream.astype(jnp.float32) + branch).astype(jnp.bfloat16)
    resid_f = resid.astype(jnp.float32)
    scale = lax.rsqrt(jnp.mean(resid_f * resid_f, axis=-1, keepdims=True) + EPSILON)
    normed = (resid_f * scale * norm_gain).astype(jnp.bfloat16)
    top_count = routes.shape[1]
    experts = gate_w.shape[0] * lax.axis_size("sp")
    capacity = max(2, own_rows * top_count * 4 // (3 * experts))
    expert_ids = jnp.arange(experts, dtype=jnp.int32)
    chosen = routes[:, :, None] == expert_ids[None, None, :]
    named = jnp.any(chosen, axis=1)
    earlier = jnp.tri(own_rows, k=-1, dtype=jnp.bfloat16)
    ranks = jnp.dot(earlier, named.astype(jnp.bfloat16), preferred_element_type=jnp.float32)
    slots = expert_ids * capacity + ranks.astype(jnp.int32)
    slot_of = jnp.sum(jnp.where(chosen, slots[:, None, :], 0), axis=2)
    slot_ids = jnp.arange(experts * capacity, dtype=jnp.int32)
    onehots = [slot_of[:, k : k + 1] == slot_ids[None, :] for k in range(top_count)]
    spread = functools.reduce(jnp.logical_or, onehots).astype(jnp.bfloat16)
    disp = lax.dot_general(
        spread, normed, (((0,), (0,)), ((), ())), preferred_element_type=jnp.float32
    ).astype(jnp.bfloat16)
    back = run_experts(disp.reshape(experts, capacity, width), gate_w, up_w, down_w)
    back_rows = back.reshape(-1, width)
    total = resid.astype(jnp.float32)
    for column in range(top_count):
        picked = jnp.dot(
            onehots[column].astype(jnp.bfloat16), back_rows, preferred_element_type=jnp.float32
        )
        total = total + route_weight[:, column : column + 1] * picked
    return total.astype(jnp.bfloat16)


def solution(mesh):
    placed = (
        P("sp", "tp"),
        P("sp", "tp"),
        P("sp", "tp"),
        P(None, "tp"),
        P("tp", None),
        P(("sp", "tp"), None),
        P(),
        P(("sp", "tp"), None),
        P(("sp", "tp"), None),
        P("sp", None, "tp"),
        P("sp", None, "tp"),
        P("sp", "tp", None),
    )
    return jax.shard_map(
        local, mesh=mesh, in_specs=placed, out_specs=P(("sp", "tp"), None), check_vma=False
    )
```

```python
import functools

import jax
import jax.numpy as jnp
from jax import lax
from jax.experimental import pallas as pl
from jax.experimental.pallas import tpu as pltpu
from jax.sharding import PartitionSpec as P

EPSILON = 1e-05
LIMIT = 7.0
ALPHA = 1.702

MESH = pl.DeviceIdType.MESH


def clamped_unit(gate_pre, up_pre):
    gated = jnp.minimum(gate_pre, LIMIT)
    upward = jnp.clip(up_pre, -LIMIT, LIMIT)
    return (upward + 1.0) * gated * jax.nn.sigmoid(ALPHA * gated)


def experts_kernel(
    n,
    group,
    disp,
    gate_w,
    up_w,
    down_w,
    out,
    rows,
    parts,
    partner_parts,
    chip_sum,
    peer_sum,
    final,
    gate_v,
    up_v,
    down_v,
    w_sem,
    own_sem,
    sp_send,
    sp_recv,
    pair_send,
    pair_recv,
    peer_send,
    peer_recv,
    fwd_send,
    fwd_recv,
    part_send,
    part_recv,
    sum_send,
    sum_recv,
    ret_send,
    ret_recv,
):
    steps = n // group
    me = lax.axis_index("sp")
    quarter = lax.axis_index("tp")
    y, c = quarter // 2, quarter % 2
    partner = {"tp": y * 2 + 1 - c}
    peer = {"tp": (1 - y) * 2 + c}

    def remote(source, target, send, recv, device):
        return pltpu.make_async_remote_copy(
            src_ref=source,
            dst_ref=target,
            send_sem=send,
            recv_sem=recv,
            device_id=device,
            device_id_type=MESH,
        )

    loads = [
        pltpu.make_async_copy(gate_w.at[0], gate_v, w_sem.at[0]),
        pltpu.make_async_copy(up_w.at[0], up_v, w_sem.at[1]),
        pltpu.make_async_copy(down_w.at[0], down_v, w_sem.at[2]),
    ]
    own_in = pltpu.make_async_copy(disp.at[me], rows.at[0, c, y, 0], own_sem.at[0])
    own_out = pltpu.make_async_copy(final.at[0, 0], out.at[me], own_sem.at[1])
    own_in.start()
    for load in loads:
        load.start()

    barrier = pltpu.get_barrier_semaphore()

    @pl.loop(1, n)
    def _(j):
        pl.semaphore_signal(barrier, inc=1, device_id={"sp": (me + j) % n}, device_id_type=MESH)

    pl.semaphore_signal(barrier, inc=1, device_id=partner, device_id_type=MESH)
    pl.semaphore_signal(barrier, inc=1, device_id=peer, device_id_type=MESH)
    pl.semaphore_wait(barrier, n + 1)

    def dispatch(j):
        to = (me + n - j) % n
        return remote(
            disp.at[to],
            rows.at[j // group, c, y, j % group],
            sp_send.at[j],
            sp_recv.at[j],
            {"sp": to},
        )

    def pair(t):
        block = rows.at[t, c, y]
        return remote(block, block, pair_send.at[t], pair_recv.at[t], partner)

    def across(t):
        block = rows.at[t, c, y]
        return remote(block, block, peer_send.at[t], peer_recv.at[t], peer)

    def forward(t):
        block = rows.at[t, c, 1 - y]
        return remote(block, block, fwd_send.at[t], fwd_recv.at[t], partner)

    def part(t):
        return remote(
            parts.at[t, 1 - c], partner_parts.at[t], part_send.at[t], part_recv.at[t], partner
        )

    def summed(t):
        return remote(chip_sum.at[t], peer_sum.at[t], sum_send.at[t], sum_recv.at[t], peer)

    def back(j):
        return remote(
            final.at[j // group, j % group],
            out.at[me],
            ret_send.at[j],
            ret_recv.at[j],
            {"sp": (me + j) % n},
        )

    @pl.loop(1, n)
    def _(j):
        dispatch(j).start()

    own_in.wait()
    for load in loads:
        load.wait()
    cap, width = rows.shape[-2:]
    count = 4 * group * cap

    def compute(t):
        x = rows[t].reshape(count, width)
        gate_pre = jnp.dot(x, gate_v[...], preferred_element_type=jnp.float32)
        up_pre = jnp.dot(x, up_v[...], preferred_element_type=jnp.float32)
        active = clamped_unit(gate_pre, up_pre).astype(jnp.bfloat16)
        tile = 512
        for at in range(0, width, tile):
            piece = jnp.dot(active, down_v[:, at : at + tile], preferred_element_type=jnp.float32)
            parts[t, :, :, :, :, at : at + tile] = piece.astype(jnp.bfloat16).reshape(
                2, 2, group, cap, tile
            )

    @pl.loop(0, steps + 4)
    def _(t):
        @pl.when(t < steps)
        def _():
            for g in range(group):
                j = t * group + g

                @pl.when(j > 0)
                def _():
                    dispatch(j).wait_recv()

            across(t).start()
            pair(t).start()

        @pl.when((t >= 1) & (t < steps + 1))
        def _():
            across(t - 1).wait_recv()
            forward(t - 1).start()

        @pl.when((t >= 2) & (t < steps + 2))
        def _():
            pair(t - 2).wait_recv()
            forward(t - 2).wait_recv()
            compute(t - 2)
            part(t - 2).start()

        @pl.when((t >= 3) & (t < steps + 3))
        def _():
            s = t - 3
            part(s).wait_recv()
            chip_sum[s] = (
                parts[s, c, 1 - y].astype(jnp.float32)
                + partner_parts[s, 1 - y].astype(jnp.float32)
            ).astype(jnp.bfloat16)
            summed(s).start()

        @pl.when(t >= 4)
        def _():
            s = t - 4
            summed(s).wait_recv()
            final[s] = (
                parts[s, c, y].astype(jnp.float32)
                + partner_parts[s, y].astype(jnp.float32)
                + peer_sum[s].astype(jnp.float32)
            ).astype(jnp.bfloat16)
            for g in range(group):
                j = s * group + g

                @pl.when(j > 0)
                def _():
                    back(j).start()

                @pl.when(j == 0)
                def _():
                    own_out.start()

    own_out.wait()

    @pl.loop(0, steps)
    def _(t):
        pair(t).wait_send()
        across(t).wait_send()
        forward(t).wait_send()
        part(t).wait_send()
        summed(t).wait_send()

    @pl.loop(1, n)
    def _(j):
        dispatch(j).wait_send()
        back(j).wait()


def run_experts(disp, gate_w, up_w, down_w):
    n, cap, width = disp.shape
    hidden = gate_w.shape[2]
    group = 1
    while n % (2 * group) == 0 and n // group > 8 and 4 * group * cap < 256:
        group *= 2
    steps = n // group
    kind = jnp.bfloat16
    hbm = pl.BlockSpec(memory_space=pltpu.HBM)
    dma = pltpu.SemaphoreType.DMA
    return pl.pallas_call(
        functools.partial(experts_kernel, n, group),
        out_shape=jax.ShapeDtypeStruct((n, cap, width), kind),
        in_specs=[hbm] * 4,
        out_specs=hbm,
        scratch_shapes=[
            pltpu.VMEM((steps, 2, 2, group, cap, width), kind),
            pltpu.VMEM((steps, 2, 2, group, cap, width), kind),
            pltpu.VMEM((steps, 2, group, cap, width), kind),
            pltpu.VMEM((steps, group, cap, width), kind),
            pltpu.VMEM((steps, group, cap, width), kind),
            pltpu.VMEM((steps, group, cap, width), kind),
            pltpu.VMEM((width, hidden), kind),
            pltpu.VMEM((width, hidden), kind),
            pltpu.VMEM((hidden, width), kind),
            dma((3,)),
            dma((2,)),
            dma((n,)),
            dma((n,)),
        ]
        + [dma((steps,))] * 10
        + [dma((n,))] * 2,
        compiler_params=pltpu.CompilerParams(
            collective_id=0, has_side_effects=True, vmem_limit_bytes=60 * 1024 * 1024
        ),
    )(disp, gate_w, up_w, down_w)


CHUNKS = 4


def mixer_kernel(
    n,
    conv_in,
    conv_pre,
    conv_post,
    taps,
    out_proj,
    stream,
    gain,
    spread,
    resid_out,
    disp_out,
    halo,
    mixed,
    regrouped,
    w_pair,
    w_peer,
    w_far,
    total,
    halo_send,
    halo_recv,
    mix_send,
    mix_recv,
    pair_send,
    pair_recv,
    peer_send,
    peer_recv,
    swap_send,
    swap_recv,
    far_send,
    far_recv,
):
    me = lax.axis_index("sp")
    quarter = lax.axis_index("tp")
    y, c = quarter // 2, quarter % 2
    partner = {"tp": y * 2 + 1 - c}
    peer = {"tp": (1 - y) * 2 + c}
    half = me % 2
    twin = {"sp": me + 1 - 2 * half}
    length, channels = conv_in.shape
    own_rows, width = stream.shape
    edge = halo.shape[1]
    depth = channels // 2 // CHUNKS

    def remote(source, target, send, recv, device):
        return pltpu.make_async_remote_copy(
            src_ref=source,
            dst_ref=target,
            send_sem=send,
            recv_sem=recv,
            device_id=device,
            device_id_type=MESH,
        )

    barrier = pltpu.get_barrier_semaphore()
    for shift in (1, n - 1):
        pl.semaphore_signal(
            barrier, inc=1, device_id={"sp": (me + shift) % n}, device_id_type=MESH
        )
    for shift in (1, 2, 3):
        pl.semaphore_signal(
            barrier, inc=1, device_id={"tp": (quarter + shift) % 4}, device_id_type=MESH
        )
    pl.semaphore_wait(barrier, 5)

    def up(k, source):
        return remote(
            source.at[length - edge : length],
            halo.at[k],
            halo_send.at[k],
            halo_recv.at[k],
            {"sp": (me + 1) % n},
        )

    def down(k, source):
        return remote(
            source.at[0:edge],
            halo.at[2 + k],
            halo_send.at[2 + k],
            halo_recv.at[2 + k],
            {"sp": (me + n - 1) % n},
        )

    def rows(h, k):
        return pl.ds((h * CHUNKS + k) * depth, depth)

    def whole():
        return remote(out_proj, w_pair, pair_send.at[0], pair_recv.at[0], partner)

    def across(k):
        at = rows(half, k)
        return remote(out_proj.at[at], w_peer.at[at], peer_send.at[k], peer_recv.at[k], peer)

    def swap(k):
        at = rows(half, k)
        return remote(w_peer.at[at], w_peer.at[at], swap_send.at[k], swap_recv.at[k], twin)

    def far(k, h, slot):
        at = rows(h, k)
        return remote(w_peer.at[at], w_far.at[at], far_send.at[slot], far_recv.at[slot], partner)

    def send_mixed(shift):
        return remote(
            mixed.at[(quarter + shift) % 4],
            regrouped.at[shift],
            mix_send.at[shift],
            mix_recv.at[shift],
            {"tp": (quarter + shift) % 4},
        )

    @pl.when(me < n - 1)
    def _():
        up(0, conv_in).start()
        up(1, conv_pre).start()

    @pl.when(me > 0)
    def _():
        down(0, conv_in).start()
        down(1, conv_pre).start()

    for k in range(CHUNKS):
        across(k).start()
    whole().start()

    @pl.when(me == 0)
    def _():
        halo[0:2] = jnp.zeros((2,) + halo.shape[1:], halo.dtype)

    @pl.when(me == n - 1)
    def _():
        halo[2:4] = jnp.zeros((2,) + halo.shape[1:], halo.dtype)

    @pl.when(me > 0)
    def _():
        up(0, conv_in).wait_recv()
        up(1, conv_pre).wait_recv()

    @pl.when(me < n - 1)
    def _():
        down(0, conv_in).wait_recv()
        down(1, conv_pre).wait_recv()

    product = conv_pre[...].astype(jnp.float32) * conv_in[...].astype(jnp.float32)
    before_rows = halo[0].astype(jnp.float32) * halo[1].astype(jnp.float32)
    after_rows = halo[2].astype(jnp.float32) * halo[3].astype(jnp.float32)
    position = lax.broadcasted_iota(jnp.int32, product.shape, 0)
    before = jnp.where(position == 0, before_rows[edge - 1 : edge], pltpu.roll(product, 1, 0))
    after = jnp.where(
        position == length - 1, after_rows[0:1], pltpu.roll(product, length - 1, 0)
    )
    convolved = taps[0:1] * before + taps[1:2] * product + taps[2:3] * after
    value = (conv_post[...].astype(jnp.float32) * convolved).astype(jnp.bfloat16)
    mixed[...] = value.reshape(mixed.shape)

    for k in range(CHUNKS):
        across(k).wait_recv()
        swap(k).start()
        far(k, half, k).start()
        if k == 0:
            for shift in (1, 2, 3):
                send_mixed(shift).start()

    total[...] = jnp.dot(mixed[quarter], out_proj[...], preferred_element_type=jnp.float32)
    whole().wait_recv()

    for k in range(CHUNKS):
        swap(k).wait_recv()
        far(k, 1 - half, CHUNKS + k).start()
    for shift in (1, 2, 3):
        send_mixed(shift).wait_recv()

    def block(of):
        return regrouped[(quarter + 4 - of) % 4]

    total[...] += jnp.dot(
        block(y * 2 + 1 - c), w_pair[...], preferred_element_type=jnp.float32
    )
    total[...] += jnp.dot(
        block((1 - y) * 2 + c), w_peer[...], preferred_element_type=jnp.float32
    )
    for k in range(CHUNKS):
        far(k, half, k).wait_recv()
        far(k, 1 - half, CHUNKS + k).wait_recv()
    branch = total[...] + jnp.dot(
        block((1 - y) * 2 + 1 - c), w_far[...], preferred_element_type=jnp.float32
    )
    resid = (stream[...].astype(jnp.float32) + branch).astype(jnp.bfloat16)
    resid_out[...] = resid
    resid_f = resid.astype(jnp.float32)
    scale = lax.rsqrt(jnp.mean(resid_f * resid_f, axis=-1, keepdims=True) + EPSILON)
    normed = (resid_f * scale * gain[...]).astype(jnp.bfloat16)
    tile = 512
    for at in range(0, width, tile):
        disp_out[:, at : at + tile] = jnp.dot(
            spread[...], normed[:, at : at + tile], preferred_element_type=jnp.float32
        ).astype(jnp.bfloat16)

    @pl.when(me < n - 1)
    def _():
        up(0, conv_in).wait_send()
        up(1, conv_pre).wait_send()

    @pl.when(me > 0)
    def _():
        down(0, conv_in).wait_send()
        down(1, conv_pre).wait_send()

    whole().wait_send()
    for k in range(CHUNKS):
        across(k).wait_send()
        swap(k).wait_send()
        far(k, half, k).wait_send()
        far(k, 1 - half, CHUNKS + k).wait_send()
    for shift in (1, 2, 3):
        send_mixed(shift).wait_send()


def run_mixer(conv_in, conv_pre, conv_post, taps, out_proj, stream, gain, spread):
    n = lax.axis_size("sp")
    own_rows, width = stream.shape
    channels = conv_in.shape[1]
    slots = spread.shape[0]
    kind = jnp.bfloat16
    vmem = pl.BlockSpec(memory_space=pltpu.VMEM)
    dma = pltpu.SemaphoreType.DMA
    return pl.pallas_call(
        functools.partial(mixer_kernel, n),
        out_shape=(
            jax.ShapeDtypeStruct((own_rows, width), kind),
            jax.ShapeDtypeStruct((slots, width), kind),
        ),
        in_specs=[vmem] * 8,
        out_specs=(vmem, vmem),
        scratch_shapes=[
            pltpu.VMEM((4, 16, channels), kind),
            pltpu.VMEM((4, own_rows, channels), kind),
            pltpu.VMEM((4, own_rows, channels), kind),
            pltpu.VMEM((channels, width), kind),
            pltpu.VMEM((channels, width), kind),
            pltpu.VMEM((channels, width), kind),
            pltpu.VMEM((own_rows, width), jnp.float32),
            dma((4,)),
            dma((4,)),
            dma((4,)),
            dma((4,)),
            dma((1,)),
            dma((1,)),
        ]
        + [dma((CHUNKS,))] * 4
        + [dma((2 * CHUNKS,))] * 2,
        compiler_params=pltpu.CompilerParams(
            collective_id=1, has_side_effects=True, vmem_limit_bytes=40000 * 1024
        ),
    )(conv_in, conv_pre, conv_post, taps, out_proj, stream, gain, spread)


def local(
    conv_in,
    conv_pre,
    conv_post,
    taps,
    out_proj,
    stream,
    norm_gain,
    routes,
    route_weight,
    gate_w,
    up_w,
    down_w,
):
    own_rows = stream.shape[0]
    width = stream.shape[1]
    top_count = routes.shape[1]
    experts = gate_w.shape[0] * lax.axis_size("sp")
    capacity = max(2, own_rows * top_count * 4 // (3 * experts))
    expert_ids = jnp.arange(experts, dtype=jnp.int32)
    chosen = routes[:, :, None] == expert_ids[None, None, :]
    named = jnp.any(chosen, axis=1)
    earlier = jnp.tri(own_rows, k=-1, dtype=jnp.bfloat16)
    ranks = jnp.dot(earlier, named.astype(jnp.bfloat16), preferred_element_type=jnp.float32)
    slots = expert_ids * capacity + ranks.astype(jnp.int32)
    slot_of = jnp.sum(jnp.where(chosen, slots[:, None, :], 0), axis=2)
    slot_ids = jnp.arange(experts * capacity, dtype=jnp.int32)
    onehots = [slot_of[:, k : k + 1] == slot_ids[None, :] for k in range(top_count)]
    spread = functools.reduce(
        jnp.logical_or, [slot_ids[:, None] == slot_of[None, :, k] for k in range(top_count)]
    ).astype(jnp.bfloat16)
    resid, disp = run_mixer(
        conv_in, conv_pre, conv_post, taps, out_proj, stream, norm_gain[None, :], spread
    )
    back = run_experts(disp.reshape(experts, capacity, width), gate_w, up_w, down_w)
    back_rows = back.reshape(-1, width)
    total = resid.astype(jnp.float32)
    for column in range(top_count):
        picked = jnp.dot(
            onehots[column].astype(jnp.bfloat16), back_rows, preferred_element_type=jnp.float32
        )
        total = total + route_weight[:, column : column + 1] * picked
    return total.astype(jnp.bfloat16)


def solution(mesh):
    placed = (
        P("sp", "tp"),
        P("sp", "tp"),
        P("sp", "tp"),
        P(None, "tp"),
        P("tp", None),
        P(("sp", "tp"), None),
        P(),
        P(("sp", "tp"), None),
        P(("sp", "tp"), None),
        P("sp", None, "tp"),
        P("sp", None, "tp"),
        P("sp", "tp", None),
    )
    return jax.shard_map(
        local, mesh=mesh, in_specs=placed, out_specs=P(("sp", "tp"), None), check_vma=False
    )
```
